256 devices in a mesh: sp: 64 (over z, x, core), tp: 4 (over y).
Axes of the slice: x: 4, y: 4, z: 8, core: 2. Of those that a mesh axis runs over, the one named last changes fastest.
Arguments:
- residual_in: bfloat16 [32768, 2048], P('sp'), may hold values from -6 to 6
- gate_in: bfloat16 [32768, 2048], P('sp', 'tp'), may hold values from -6 to 6
- value_in: bfloat16 [32768, 2048], P('sp', 'tp'), may hold values from -6 to 6
- conv_weight: float32 [4, 2048], P(None, 'tp'), may hold values from -3 to 3
- rate_weight: bfloat16 [32, 64, 64], P('tp'), may hold values from -0.75 to 0.75
- input_weight: bfloat16 [32, 64, 64], P('tp'), may hold values from -0.75 to 0.75
- decay_base: float32 [2048], P('tp'), may hold values from 3.8146973e-07 to 0.015, as said below
- step_scale: float32 [32768, 2048], P('sp', 'tp'), may hold values from 0.25 to 458752, as said below
- out_weight: bfloat16 [2048, 2048], P('tp'), may hold values from -0.375 to 0.375
- norm_gain: float32 [2048], replicated, may hold values from 0.1 to 1.9
- up_weight: bfloat16 [2048, 8192], P('sp', 'tp'), may hold values from -0.125 to 0.125
- down_weight: bfloat16 [2048, 8192], P('sp', 'tp'), may hold values from -0.0625 to 0.0625
Outputs:
- block_out: bfloat16 [32768, 2048], P(('sp', 'tp'))
The draws below stay inside these ranges and needn't reach their ends.
Inputs may be any that keep to these rules, and one draw needn't show every extreme that they name: `decay_base`: positive. `step_scale`: positive.
All inputs are finite; a program needn't handle non-finite values.
Results may differ from the reference program's by a relative error of at most 0.018.
Values may be sent and summed in bfloat16 or wider, within the bound.
A program may use at most 128 MiB of HBM per device.

```python
import jax
import jax.numpy as jnp
from jax import lax

D = 2048
BW = 64
FF = 8192
CONV = 4
TOK_DEV = 512
R = 2048
BLOCKS = 32
RCH = 512
FCH = 2048
TOKENS = 32768
N_TP = 4


def channel_law(key):
    base_key = jax.random.fold_in(key, 11)
    pick_key, slow_key, fast_key = jax.random.split(base_key, 3)
    slow_mask = jax.random.bernoulli(pick_key, 0.5, (R,))
    slow_rate = jax.random.uniform(slow_key, (R,), jnp.float32, 0.05, 0.5) / (4.0 * TOKENS)
    fast_rate = jax.random.uniform(fast_key, (R,), jnp.float32, 0.005, 0.015)
    return jnp.where(slow_mask, slow_rate, fast_rate)


def draw_decay_base(key, part):
    return channel_law(key)


def draw_step_scale(key, part):
    per_channel_rate = channel_law(key)
    scale_key = jax.random.fold_in(key, 23)
    level_key, rough_key, spot_key, loss_key = jax.random.split(scale_key, 4)
    block_total = TOKENS // TOK_DEV
    noise_level = jnp.exp(jax.random.uniform(level_key, (block_total, 1), jnp.float32, -0.6931, 0.6931))
    noise_level = jnp.repeat(noise_level, TOK_DEV, axis=0)
    noisy_input = jax.random.uniform(rough_key, (TOKENS, R), jnp.float32, 0.5, 1.5)
    spots = jax.random.randint(spot_key, (8,), 0, TOKENS)
    flagged_rows = jnp.zeros((TOKENS,), jnp.float32).at[spots].set(1.0)
    training_loss = jax.random.uniform(loss_key, (TOKENS, R), jnp.float32, 0.25, 0.7)
    spike_draw = training_loss / (4.0 * per_channel_rate[None, :])
    return jnp.where(flagged_rows[:, None] > 0.5, spike_draw, noise_level * noisy_input)


def block_levels(key, shape, pieces, smallest, top_value):
    def one(dim, parts):
        steps = jax.random.uniform(jax.random.fold_in(jax.random.fold_in(key, 6), dim), (parts,), jnp.float32, smallest / len(pieces), top_value / len(pieces))
        return jnp.repeat(jnp.exp(steps), shape[dim] // parts).reshape((-1,) + (1,) * (len(shape) - dim - 1))

    gain = one(*pieces[0])
    for cut in pieces[1:]:
        gain = gain * one(*cut)
    return gain


def bell_draw(stream_key, dims, deviation, reach, cuts=(), kind=jnp.bfloat16):
    result = jax.random.normal(stream_key, dims, jnp.float32) * deviation
    if len(cuts) > 0:
        result = block_levels(stream_key, dims, cuts, -0.22, 0.18) * result
    return jnp.clip(result, min=-reach, max=reach).astype(kind)


def setup_inputs(seed: int = 0) -> dict:
    key_list = jax.random.split(jax.random.key(seed), 13)
    return {
        "residual_in": bell_draw(key_list[0], (TOKENS, D), 1.0, 6.0, ((0, 64),)),
        "gate_in": bell_draw(key_list[1], (TOKENS, R), 1.0, 6.0, ((0, 64), (1, 4))),
        "value_in": bell_draw(key_list[2], (TOKENS, R), 1.0, 6.0, ((0, 64), (1, 4))),
        "conv_weight": bell_draw(key_list[3], (CONV, R), CONV ** -0.5, 3.0, ((1, 4),), jnp.float32),
        "rate_weight": bell_draw(key_list[4], (BLOCKS, BW, BW), BW ** -0.5, 0.75, ((0, 4),)),
        "input_weight": bell_draw(key_list[5], (BLOCKS, BW, BW), BW ** -0.5, 0.75, ((0, 4),)),
        "decay_base": draw_decay_base(jax.random.fold_in(key_list[12], 71), 0),
        "step_scale": draw_step_scale(jax.random.fold_in(key_list[12], 71), 0),
        "out_weight": bell_draw(key_list[8], (R, D), (R // 8) ** -0.5, 0.375, ((0, 4),)),
        "norm_gain": jnp.clip(1.0 + 0.18 * jax.random.normal(key_list[9], (D,), jnp.float32), 0.1, 1.9),
        "up_weight": bell_draw(key_list[10], (D, FF), D ** -0.5, 0.125, ((0, 64), (1, 4))),
        "down_weight": bell_draw(key_list[11], (D, FF), FF ** -0.5, 0.0625, ((0, 64), (1, 4))),
    }


def chain_join(earlier, later):
    return (earlier[0] * later[0], later[0] * earlier[1] + later[1])

def rounded(term):
    return lax.optimization_barrier(term.astype(jnp.bfloat16)).astype(jnp.float32)

def reference(residual_in, gate_in, value_in, conv_weight, rate_weight, input_weight, decay_base, step_scale, out_weight, norm_gain, up_weight, down_weight):
    tap_count = conv_weight.shape[0]
    total_rows = value_in.shape[0]
    padded = jnp.pad(value_in.astype(jnp.float32), ((tap_count - 1, 0), (0, 0)))
    filtered_rows = jnp.zeros(value_in.shape, jnp.float32)
    for offset in range(tap_count):
        filtered_rows = filtered_rows + padded[offset:offset + total_rows] * conv_weight[offset]
    smoothed = filtered_rows.astype(jnp.bfloat16)
    grouped = smoothed.astype(jnp.float32).reshape(total_rows, BLOCKS, BW)
    rate_gate = jax.nn.sigmoid(jnp.einsum('tnd,nde->tne', grouped, rate_weight.astype(jnp.float32))).reshape(total_rows, R)
    input_gate = jax.nn.sigmoid(jnp.einsum('tnd,nde->tne', grouped, input_weight.astype(jnp.float32))).reshape(total_rows, R)
    log_keep = -8.0 * step_scale * rate_gate * decay_base[None, :]
    drive = jnp.sqrt(-jnp.expm1(2.0 * log_keep)) * input_gate * smoothed.astype(jnp.float32)
    products, carry_state = lax.associative_scan(chain_join, (jnp.exp(log_keep), drive), axis=0)
    gated = (jax.nn.gelu(gate_in.astype(jnp.float32), approximate=True) * carry_state).astype(jnp.bfloat16)
    mixed = jnp.zeros((total_rows, D), jnp.float32)
    for group in range(N_TP):
        part_sum = jnp.dot(gated[:, group * RCH:(group + 1) * RCH], out_weight[group * RCH:(group + 1) * RCH], preferred_element_type=jnp.float32)
        mixed = mixed + rounded(part_sum)
    updated = (residual_in.astype(jnp.float32) + mixed).astype(jnp.bfloat16)
    widened = updated.astype(jnp.float32)
    factor = lax.rsqrt(lax.optimization_barrier(jnp.mean(widened * widened, axis=-1, keepdims=True)) + 1e-06)
    normed = (widened * factor * norm_gain).astype(jnp.bfloat16)
    down_sum = jnp.zeros((total_rows, D), jnp.float32)
    for group in range(N_TP):
        lifted = jnp.dot(normed, up_weight[:, group * FCH:(group + 1) * FCH], preferred_element_type=jnp.float32)
        activated = jnp.square(jax.nn.relu(lifted)).astype(jnp.bfloat16)
        part_sum = lax.dot_general(activated, down_weight[:, group * FCH:(group + 1) * FCH], (((1,), (1,)), ((), ())), preferred_element_type=jnp.float32)
        down_sum = down_sum + rounded(part_sum)
    return (updated.astype(jnp.float32) + down_sum).astype(jnp.bfloat16)
```

```python
import jax
import jax.numpy as jnp
from jax import lax
from jax.experimental import pallas as pl
from jax.experimental.pallas import tpu as pltpu
from jax.sharding import Mesh
from jax.sharding import PartitionSpec as P

MESH = pl.DeviceIdType.MESH
SP = ("z", "x", "c")
SP_TP = ("z", "x", "c", "y")
NZ, NX, NC, NY = 8, 4, 2, 4
ROWS = 512
CH = 512
D = 2048
F = 2048
SEG = 64
HALF = 1024
TILE = 256
N_COPIES = 160
F32 = jnp.float32
BF16 = jnp.bfloat16


class Copies:
    def __init__(self, send, recv):
        self.send, self.recv, self.made = send, recv, []

    def go(self, src, dst, device):
        k = len(self.made)
        assert k < N_COPIES
        copy = pltpu.make_async_remote_copy(
            src_ref=src,
            dst_ref=dst,
            send_sem=self.send.at[k],
            recv_sem=self.recv.at[k],
            device_id=device,
            device_id_type=MESH,
        )
        copy.start()
        self.made.append(copy)
        return copy

    def finish(self):
        for copy in self.made:
            copy.wait_send()


def one_minus_exp(y):
    poly = 1.0 - y * (1.0 / 9.0)
    for k in range(8, 1, -1):
        poly = 1.0 - y * (1.0 / k) * poly
    return y * poly


def kernel(
    residual_hbm,
    gate_hbm,
    value_hbm,
    conv_hbm,
    rate_hbm,
    input_hbm,
    decay_hbm,
    step_hbm,
    out_w_hbm,
    gain_hbm,
    up_hbm,
    down_hbm,
    result_hbm,
    value,
    gate,
    step,
    conv,
    rate_w,
    input_w,
    decay,
    out_w,
    gain,
    residual,
    up_w,
    down_w,
    gate_pair,
    keep,
    drive,
    gelu,
    entry_p,
    entry_s,
    pay,
    plane,
    pay_z,
    column,
    gated,
    mixed,
    normed,
    act,
    part,
    first_l,
    first_r,
    comb_l,
    comb_r,
    from_dn,
    from_up,
    updated,
    result,
    local_sem,
    send_sem,
    recv_sem,
):
    z = lax.axis_index("z")
    x = lax.axis_index("x")
    c = lax.axis_index("c")
    y = lax.axis_index("y")

    loads = {}

    def load(name, src, dst):
        copy = pltpu.make_async_copy(src, dst, local_sem.at[len(loads)])
        copy.start()
        loads[name] = copy

    load("value", value_hbm, value.at[pl.ds(16, ROWS)])
    load("up", up_hbm, up_w.at[z, x, c])
    load("down", down_hbm, down_w.at[z, x, c])
    load("rate", rate_hbm, rate_w)
    load("input", input_hbm, input_w)
    load("conv", conv_hbm, conv)
    load("decay", decay_hbm, decay)
    load("step", step_hbm, step)
    load("gate", gate_hbm, gate)
    load("out_w", out_w_hbm, out_w)
    load("gain", gain_hbm, gain)
    load("residual", residual_hbm.at[pl.ds(pl.multiple_of(y * 128, 128), 128)], residual)

    here = {"z": z, "x": x, "c": c, "y": y}

    def at(**other):
        return {**here, **other}

    line = (z * NX + x) * NC + c

    def on_line(k):
        return at(z=k // (NX * NC), x=(k // NC) % NX, c=k % NC)

    x_up, x_dn = at(x=(x + 1) % NX), at(x=(x + NX - 1) % NX)
    z_up, z_dn = at(z=(z + 1) % NZ), at(z=(z + NZ - 1) % NZ)
    y_up_k, y_dn_k, y_op_k = (y + 1) % NY, (y + NY - 1) % NY, (y + 2) % NY
    y_up, y_dn = at(y=y_up_k), at(y=y_dn_k)
    partner = at(c=1 - c)
    next_row = on_line((line + 1) % (NZ * NX * NC))
    prev_row = on_line((line + NZ * NX * NC - 1) % (NZ * NX * NC))
    plane_peers = [
        at(x=(x + dx) % NX, c=(c + dc) % NC) for dx in range(NX) for dc in range(NC) if dx or dc
    ]
    column_peers = [at(z=(z + dz) % NZ) for dz in range(1, NZ)]
    greeted = [next_row, prev_row, y_up, y_dn, *plane_peers, *column_peers]
    barrier = pltpu.get_barrier_semaphore()
    for device in greeted:
        pl.semaphore_signal(barrier, inc=1, device_id=device, device_id_type=MESH)

    copies = Copies(send_sem, recv_sem)
    go = copies.go

    loads["value"].wait()
    loads["up"].wait()
    loads["down"].wait()
    pl.semaphore_wait(barrier, len(greeted))

    halo = go(value.at[pl.ds(ROWS, 16)], value.at[pl.ds(0, 16)], next_row)

    swaps = []

    def swap(ref):
        swaps.append(go(ref, ref, partner))

    def zz(distance):
        return (z + NZ + distance) % NZ

    def xx(distance):
        return (x + NX + distance) % NX

    own_up = up_w.at[z, x, c]
    own_down = down_w.at[z, x, c]
    up_x = [go(own_up, own_up, x_up), go(own_up, own_up, x_dn)]
    down_z = {(1, 0): go(own_down, own_down, z_up), (1, 1): go(own_down, own_down, z_dn)}
    up_z = {}
    down_x = {}

    def event_up_x1():
        up_x[0].wait_recv()
        ref = up_w.at[z, xx(-1), c, pl.ds(0, 16)]
        up_x.append(go(ref, ref, x_up))
        up_x[1].wait_recv()
        ref = up_w.at[z, xx(1), c, pl.ds(16, 16)]
        up_x.append(go(ref, ref, x_dn))

    def event_up_x2():
        up_x[2].wait_recv()
        up_x[3].wait_recv()
        for h in range(2):
            ref = up_w.at[z, pl.ds(2 * h, 2), c]
            up_z[1, h, 0] = go(ref, ref, z_up)
            up_z[1, h, 1] = go(ref, ref, z_dn)
        swap(up_w.at[z, :, c])

    def event_up_z(d, h):
        def run():
            for way, device, sign in ((0, z_up, -1), (1, z_dn, 1)):
                if (d, h, way) not in up_z:
                    continue
                up_z[d, h, way].wait_recv()
                ref = up_w.at[zz(sign * d), pl.ds(2 * h, 2), c]
                if d < 3 or (d == 3 and h == way):
                    up_z[d + 1, h, way] = go(ref, ref, device)
                swap(ref)

        return run

    def start_down_x(k, zk):
        ref = down_w.at[zk, x, c]
        down_x[k] = [go(ref, ref, x_up), go(ref, ref, x_dn), zk]

    def event_down_z(d):
        def run():
            for way, device, sign in ((0, z_up, -1), (1, z_dn, 1)):
                down_z[d, way].wait_recv()
                source = zz(sign * d)
                if d < 3:
                    ref = down_w.at[source, x, c]
                    down_z[d + 1, way] = go(ref, ref, device)
                elif d == 3:
                    ref = down_w.at[source, x, c, pl.ds(16 * way, 16)]
                    down_z[d + 1, way] = go(ref, ref, device)
                if d < 4:
                    start_down_x(2 * d - 1 + way, source)
            if d == 4:
                start_down_x(7, zz(4))

        return run

    def event_down_x(k):
        def run():
            first, second, zk = down_x[k]
            first.wait_recv()
            if k % 2 == 0:
                ref = down_w.at[zk, xx(-1), c]
                last = go(ref, ref, x_up)
            second.wait_recv()
            if k % 2 == 1:
                ref = down_w.at[zk, xx(1), c]
                last = go(ref, ref, x_dn)
            down_x[k].append(last)

        return run

    def event_down_x2(k):
        def run():
            down_x[k][3].wait_recv()
            swap(down_w.at[down_x[k][2], :, c])

        return run

    start_down_x(0, z)
    events = [
        event_up_x1,
        event_down_z(1),
        event_up_x2,
        event_down_x(0),
        event_down_z(2),
        event_down_x2(0),
        event_down_x(1),
        event_down_z(3),
        event_up_z(1, 0),
        event_down_x2(1),
        event_down_x(2),
        event_down_z(4),
        event_up_z(1, 1),
        event_down_x2(2),
        event_down_x(3),
        event_up_z(2, 0),
        event_down_x2(3),
        event_down_x(4),
        event_up_z(2, 1),
        event_down_x2(4),
        event_down_x(5),
        event_up_z(3, 0),
        event_down_x2(5),
        event_down_x(6),
        event_up_z(3, 1),
        event_down_x2(6),
        event_down_x(7),
        event_down_x2(7),
        event_up_z(4, 0),
        event_up_z(4, 1),
    ]

    def pump(count):
        for _ in range(count):
            if events:
                events.pop(0)()

    loads["rate"].wait()
    loads["input"].wait()
    loads["conv"].wait()
    loads["decay"].wait()
    loads["step"].wait()
    empty = jnp.zeros((64, 64), BF16)
    for g in range(4):
        top = [rate_w[2 * g], empty, input_w[2 * g], empty]
        low = [empty, rate_w[2 * g + 1], empty, input_w[2 * g + 1]]
        gate_pair[g, 0:64, :] = jnp.concatenate(top, axis=1)
        gate_pair[g, 64:128, :] = jnp.concatenate(low, axis=1)

    def gates(block):
        start = pl.multiple_of(block * SEG, SEG)
        for g in range(4):
            lanes = pl.ds(g * 128, 128)
            window = value[pl.ds(start, SEG + 16), lanes].astype(F32)
            filtered = jnp.zeros((SEG, 128), F32)
            for tap in range(4):
                back = 3 - tap
                moved = pltpu.roll(window, back, 0) if back else window
                filtered = filtered + moved[16:] * conv[tap : tap + 1, lanes]
            smoothed = filtered.astype(BF16)
            logits = jnp.dot(smoothed, gate_pair[g], preferred_element_type=F32)
            rate = jax.nn.sigmoid(logits[:, :128])
            admit = jax.nn.sigmoid(logits[:, 128:])
            rows = pl.ds(start, SEG)
            log_keep = -8.0 * step[rows, lanes] * rate * decay[0:1, lanes]
            kept = jnp.exp(log_keep)
            lost = -2.0 * log_keep
            gap = jnp.where(lost < 0.5, one_minus_exp(jnp.minimum(lost, 0.5)), 1.0 - kept * kept)
            keep[g, rows, :] = kept
            drive[g, rows, :] = jnp.sqrt(gap) * admit * smoothed.astype(F32)

    def gates_step(block, carry):
        gates(block)
        return carry

    lax.fori_loop(1, ROWS // SEG, gates_step, 0)
    halo.wait_recv()

    @pl.when(line == 0)
    def _():
        value[0:16, :] = jnp.zeros((16, CH), BF16)

    gates(0)
    pump(1)

    def scan_step(t, carry):
        rows = pl.ds(t, 8, stride=SEG)
        after = []
        for g in range(4):
            product, state = carry[g]
            kept = keep[g, rows, :]
            product = product * kept
            state = kept * state + drive[g, rows, :]
            keep[g, rows, :] = product
            drive[g, rows, :] = state
            after.append((product, state))
        return tuple(after)

    fresh_carry = (jnp.ones((8, 128), F32), jnp.zeros((8, 128), F32))
    ends = lax.fori_loop(0, SEG, scan_step, (fresh_carry,) * 4, unroll=4)
    for g in range(4):
        product, state = ends[g]
        total_p, total_s = jnp.ones((1, 128), F32), jnp.zeros((1, 128), F32)
        for s in range(8):
            entry_p[g, s : s + 1, :] = total_p
            entry_s[g, s : s + 1, :] = total_s
            total_s = product[s : s + 1] * total_s + state[s : s + 1]
            total_p = total_p * product[s : s + 1]
        pay[g : g + 1, :] = total_p
        pay[g + 4 : g + 5, :] = total_s

    own_plane = x * NC + c
    plane[own_plane] = pay[...]
    in_plane = [go(pay, plane.at[own_plane], device) for device in plane_peers]
    pump(2)
    loads["gate"].wait()

    def gelu_step(block, carry):
        rows = pl.ds(pl.multiple_of(block * SEG, SEG), SEG)
        gelu[rows, :] = jax.nn.gelu(gate[rows, :].astype(F32), approximate=True)
        return carry

    lax.fori_loop(0, ROWS // SEG, gelu_step, 0)
    for copy in in_plane:
        copy.wait_recv()

    def prefix(pieces, size, index):
        run_p, run_s = jnp.ones((4, 128), F32), jnp.zeros((4, 128), F32)
        before_p, before_s = run_p, run_s
        for k in range(size):
            before_p = jnp.where(k == index, run_p, before_p)
            before_s = jnp.where(k == index, run_s, before_s)
            piece = pieces[k]
            run_s = piece[0:4] * run_s + piece[4:8]
            run_p = run_p * piece[0:4]
        return before_p, before_s, run_p, run_s

    inside_p, inside_s, run_p, run_s = prefix(plane, NX * NC, own_plane)
    pay_z[0:4, :] = run_p
    pay_z[4:8, :] = run_s
    column[z] = pay_z[...]
    in_column = [go(pay_z, column.at[z], device) for device in column_peers]
    pump(1)
    for copy in in_column:
        copy.wait_recv()
    _, outer_s, _, _ = prefix(column, NZ, z)
    carried = inside_p * outer_s + inside_s
    for g in range(4):
        entry_s[g] = entry_s[g] + entry_p[g] * carried[g : g + 1]

    for s in range(8):
        rows = pl.ds(s * SEG, SEG)
        for g in range(4):
            lanes = pl.ds(g * 128, 128)
            hidden = drive[g, rows, :] + keep[g, rows, :] * entry_s[g, s : s + 1, :]
            gated[s % 2, s // 2, :, lanes] = (gelu[rows, lanes] * hidden).astype(BF16)

    left, right = pl.ds(0, HALF), pl.ds(HALF, HALF)

    def scatter_start(pieces, slot):
        return {
            "l1": go(pieces.at[y_op_k, :, left], first_l.at[slot], y_dn),
            "r1": go(pieces.at[y_op_k, :, right], first_r.at[slot], y_up),
            "l0": go(pieces.at[y_up_k, :, left], from_dn.at[slot, :, left], y_up),
            "r0": go(pieces.at[y_dn_k, :, right], from_up.at[slot, :, right], y_dn),
        }

    def scatter_pass(pieces, slot, ring):
        ring["l1"].wait_recv()
        comb_l[slot] = (
            pieces[y_dn_k, :, left].astype(F32) + first_l[slot].astype(F32)
        ).astype(BF16)
        ring["l2"] = go(comb_l.at[slot], from_up.at[slot, :, left], y_dn)
        ring["r1"].wait_recv()
        comb_r[slot] = (
            pieces[y_up_k, :, right].astype(F32) + first_r[slot].astype(F32)
        ).astype(BF16)
        ring["r2"] = go(comb_r.at[slot], from_dn.at[slot, :, right], y_up)

    def scatter_end(pieces, slot, ring):
        for name in ("l0", "r0", "l2", "r2"):
            ring[name].wait_recv()
        return (
            pieces[y].astype(F32) + from_dn[slot].astype(F32) + from_up[slot].astype(F32)
        )

    def gather_start(rows):
        l, r = rows.at[y, :, left], rows.at[y, :, right]
        return [go(l, l, y_up), go(r, r, y_dn), go(r, r, y_up), go(l, l, y_dn)]

    def gather_pass(rows, ring):
        ring[0].wait_recv()
        ref = rows.at[y_dn_k, :, left]
        ring.append(go(ref, ref, y_up))
        ring[1].wait_recv()
        ref = rows.at[y_up_k, :, right]
        ring.append(go(ref, ref, y_dn))

    def gather_end(ring):
        for copy in ring[2:]:
            copy.wait_recv()

    loads["out_w"].wait()

    def project(q):
        rows = gated[q].reshape(4 * SEG, CH)

        def tile_step(n, carry):
            cols = pl.ds(pl.multiple_of(n * TILE, TILE), TILE)
            tile = jnp.dot(rows, out_w[:, cols], preferred_element_type=F32).astype(BF16)
            mixed[q, :, :, cols] = tile.reshape(4, SEG, TILE)
            return carry

        lax.fori_loop(0, D // TILE, tile_step, 0)

    def settle(q, ring):
        total = scatter_end(mixed.at[q], q, ring)
        fresh = (residual[pl.ds(q * SEG, SEG), :].astype(F32) + total).astype(BF16)
        updated[pl.ds(q * SEG, SEG), :] = fresh
        wide = fresh.astype(F32)
        factor = lax.rsqrt(jnp.mean(wide * wide, axis=-1, keepdims=True) + 1e-06)
        normed[q, y] = (wide * factor * gain[...]).astype(BF16)

    loads["residual"].wait()
    loads["gain"].wait()
    project(0)
    ring0 = scatter_start(mixed.at[0], 0)
    project(1)
    pump(2)
    scatter_pass(mixed.at[0], 0, ring0)
    ring1 = scatter_start(mixed.at[1], 1)
    pump(6)
    settle(0, ring0)
    gather0 = gather_start(normed.at[0])
    scatter_pass(mixed.at[1], 1, ring1)
    pump(6)
    gather_pass(normed.at[0], gather0)
    settle(1, ring1)
    gather1 = gather_start(normed.at[1])
    pump(6)
    gather_end(gather0)
    gather_pass(normed.at[1], gather1)
    pump(100)
    for copy in swaps:
        copy.wait_recv()

    def feed(q):
        rows = normed[q].reshape(4 * SEG, D)

        def up_step(n, carry):
            cols = pl.ds(pl.multiple_of(n * TILE, TILE), TILE)
            weight = up_w[:, :, :, :, cols].reshape(D, TILE)
            lifted = jnp.maximum(jnp.dot(rows, weight, preferred_element_type=F32), 0.0)
            act[:, cols] = (lifted * lifted).astype(BF16)
            return carry

        lax.fori_loop(0, F // TILE, up_step, 0)
        lhs = act[...]

        def down_step(n, carry):
            cols = pl.ds(pl.multiple_of(n * TILE, TILE), TILE)
            weight = down_w[n].reshape(TILE, F)
            tile = lax.dot_general(
                lhs, weight, (((1,), (1,)), ((), ())), preferred_element_type=F32
            )
            part[q, :, :, cols] = tile.astype(BF16).reshape(4, SEG, TILE)
            return carry

        lax.fori_loop(0, D // TILE, down_step, 0)

    def close(q, ring):
        total = scatter_end(part.at[q], 2 + q, ring)
        rows = pl.ds(q * SEG, SEG)
        result[rows, :] = (updated[rows, :].astype(F32) + total).astype(BF16)

    feed(0)
    ring2 = scatter_start(part.at[0], 2)
    gather_end(gather1)
    feed(1)
    scatter_pass(part.at[0], 2, ring2)
    ring3 = scatter_start(part.at[1], 3)
    close(0, ring2)
    scatter_pass(part.at[1], 3, ring3)
    close(1, ring3)
    store = pltpu.make_async_copy(result, result_hbm, local_sem.at[len(loads)])
    store.start()
    copies.finish()
    store.wait()


def local(
    residual_in,
    gate_in,
    value_in,
    conv_weight,
    rate_weight,
    input_weight,
    decay_base,
    step_scale,
    out_weight,
    norm_gain,
    up_weight,
    down_weight,
):
    vmem = pltpu.VMEM
    scratch = [
        vmem((ROWS + 16, CH), BF16),
        vmem((ROWS, CH), BF16),
        vmem((ROWS, CH), F32),
        vmem((4, CH), F32),
        vmem((8, 64, 64), BF16),
        vmem((8, 64, 64), BF16),
        vmem((1, CH), F32),
        vmem((CH, D), BF16),
        vmem((1, D), F32),
        vmem((128, D), BF16),
        vmem((NZ, NX, NC, 32, F), BF16),
        vmem((NZ, NX, NC, 32, F), BF16),
        vmem((4, 128, 256), BF16),
        vmem((4, ROWS, 128), F32),
        vmem((4, ROWS, 128), F32),
        vmem((ROWS, CH), F32),
        vmem((4, 8, 128), F32),
        vmem((4, 8, 128), F32),
        vmem((8, 128), F32),
        vmem((NX * NC, 8, 128), F32),
        vmem((8, 128), F32),
        vmem((NZ, 8, 128), F32),
        vmem((2, 4, SEG, CH), BF16),
        vmem((2, 4, SEG, D), BF16),
        vmem((2, 4, SEG, D), BF16),
        vmem((4 * SEG, F), BF16),
        vmem((2, 4, SEG, D), BF16),
        vmem((4, SEG, HALF), BF16),
        vmem((4, SEG, HALF), BF16),
        vmem((4, SEG, HALF), BF16),
        vmem((4, SEG, HALF), BF16),
        vmem((4, SEG, D), BF16),
        vmem((4, SEG, D), BF16),
        vmem((128, D), BF16),
        vmem((128, D), BF16),
        pltpu.SemaphoreType.DMA((16,)),
        pltpu.SemaphoreType.DMA((N_COPIES,)),
        pltpu.SemaphoreType.DMA((N_COPIES,)),
    ]
    return pl.pallas_call(
        kernel,
        out_shape=jax.ShapeDtypeStruct((128, D), BF16),
        in_specs=[pl.BlockSpec(memory_space=pl.ANY)] * 12,
        out_specs=pl.BlockSpec(memory_space=pl.ANY),
        scratch_shapes=scratch,
        compiler_params=pltpu.CompilerParams(
            collective_id=0, has_side_effects=True, vmem_limit_bytes=62 * 1024 * 1024
        ),
    )(
        residual_in,
        gate_in,
        value_in,
        conv_weight,
        rate_weight,
        input_weight,
        decay_base.reshape(1, -1),
        step_scale,
        out_weight,
        norm_gain.reshape(1, -1),
        up_weight,
        down_weight,
    )


def solution(mesh):
    split = Mesh(mesh.devices.reshape(NZ, NX, NC, NY), ("z", "x", "c", "y"))
    return jax.shard_map(
        local,
        mesh=split,
        in_specs=(
            P(SP, None),
            P(SP, "y"),
            P(SP, "y"),
            P(None, "y"),
            P("y", None, None),
            P("y", None, None),
            P("y"),
            P(SP, "y"),
            P("y", None),
            P(),
            P(SP, "y"),
            P(SP, "y"),
        ),
        out_specs=P(SP_TP, None),
        check_vma=False,
    )
```

```python
import jax
import jax.numpy as jnp
from jax import lax
from jax.experimental import pallas as pl
from jax.experimental.pallas import tpu as pltpu
from jax.sharding import Mesh
from jax.sharding import PartitionSpec as P

MESH = pl.DeviceIdType.MESH
scope = jax.named_scope
SP = ("z", "x", "c")
SP_TP = ("z", "x", "c", "y")
NZ, NX, NC, NY = 8, 4, 2, 4
ROWS = 512
CH = 512
D = 2048
F = 2048
SEG = 64
PITCH = SEG + 8
HALF = 1024
TILE = 512
N_COPIES = 160
F32 = jnp.float32
BF16 = jnp.bfloat16


class Copies:
    def __init__(self, send, recv):
        self.send, self.recv, self.made = send, recv, []

    def go(self, src, dst, device):
        k = len(self.made)
        assert k < N_COPIES
        copy = pltpu.make_async_remote_copy(
            src_ref=src,
            dst_ref=dst,
            send_sem=self.send.at[k],
            recv_sem=self.recv.at[k],
            device_id=device,
            device_id_type=MESH,
        )
        copy.start()
        self.made.append(copy)
        return copy

    def finish(self):
        for copy in self.made:
            copy.wait_send()


def one_minus_exp(y):
    poly = 1.0 - y * (1.0 / 9.0)
    for k in range(8, 1, -1):
        poly = 1.0 - y * (1.0 / k) * poly
    return y * poly


def kernel(
    residual_hbm,
    gate_hbm,
    value_hbm,
    conv_hbm,
    rate_hbm,
    input_hbm,
    decay_hbm,
    step_hbm,
    out_w_hbm,
    gain_hbm,
    up_hbm,
    down_hbm,
    result_hbm,
    value,
    gate,
    step,
    conv,
    rate_w,
    input_w,
    decay,
    out_w,
    gain,
    residual,
    up_w,
    down_w,
    gate_pair,
    keep,
    drive,
    gelu,
    entry_p,
    entry_s,
    pay,
    plane,
    pay_z,
    column,
    gated,
    mixed,
    normed,
    act,
    part,
    first_l,
    first_r,
    comb_l,
    comb_r,
    from_dn,
    from_up,
    updated,
    result,
    local_sem,
    send_sem,
    recv_sem,
):
    z = lax.axis_index("z")
    x = lax.axis_index("x")
    c = lax.axis_index("c")
    y = lax.axis_index("y")

    loads = {}

    def load(name, src, dst):
        copy = pltpu.make_async_copy(src, dst, local_sem.at[len(loads)])
        copy.start()
        loads[name] = copy

    load("value", value_hbm, value.at[pl.ds(16, ROWS)])
    load("up", up_hbm, up_w.at[z, x, c])
    load("down", down_hbm, down_w.at[z, x, c])
    load("rate", rate_hbm, rate_w)
    load("input", input_hbm, input_w)
    load("conv", conv_hbm, conv)
    load("decay", decay_hbm, decay)
    load("step", step_hbm, step)
    load("gate", gate_hbm, gate)
    load("out_w", out_w_hbm, out_w)
    load("gain", gain_hbm, gain)
    load("residual", residual_hbm.at[pl.ds(pl.multiple_of(y * 128, 128), 128)], residual)

    here = {"z": z, "x": x, "c": c, "y": y}

    def at(**other):
        return {**here, **other}

    line = (z * NX + x) * NC + c

    def on_line(k):
        return at(z=k // (NX * NC), x=(k // NC) % NX, c=k % NC)

    x_up, x_dn = at(x=(x + 1) % NX), at(x=(x + NX - 1) % NX)
    z_up, z_dn = at(z=(z + 1) % NZ), at(z=(z + NZ - 1) % NZ)
    y_up_k, y_dn_k, y_op_k = (y + 1) % NY, (y + NY - 1) % NY, (y + 2) % NY
    y_up, y_dn = at(y=y_up_k), at(y=y_dn_k)
    partner = at(c=1 - c)
    next_row = on_line((line + 1) % (NZ * NX * NC))
    prev_row = on_line((line + NZ * NX * NC - 1) % (NZ * NX * NC))
    plane_peers = [
        at(x=(x + dx) % NX, c=(c + dc) % NC) for dx in range(NX) for dc in range(NC) if dx or dc
    ]
    column_peers = [at(z=(z + dz) % NZ) for dz in range(1, NZ)]
    greeted = [next_row, prev_row, y_up, y_dn, *plane_peers, *column_peers]
    barrier = pltpu.get_barrier_semaphore()
    for device in greeted:
        pl.semaphore_signal(barrier, inc=1, device_id=device, device_id_type=MESH)

    copies = Copies(send_sem, recv_sem)
    go = copies.go

    loads["value"].wait()
    loads["rate"].wait()
    loads["input"].wait()
    loads["conv"].wait()
    loads["decay"].wait()
    loads["step"].wait()
    empty = jnp.zeros((64, 64), BF16)
    for g in range(4):
        top = [rate_w[2 * g], empty, input_w[2 * g], empty]
        low = [empty, rate_w[2 * g + 1], empty, input_w[2 * g + 1]]
        gate_pair[g, 0:64, :] = jnp.concatenate(top, axis=1)
        gate_pair[g, 64:128, :] = jnp.concatenate(low, axis=1)

    def gates(block):
        start = pl.multiple_of(block * SEG, SEG)
        for g in range(4):
            lanes = pl.ds(g * 128, 128)
            window = value[pl.ds(start, SEG + 16), lanes].astype(F32)
            filtered = jnp.zeros((SEG, 128), F32)
            for tap in range(4):
                back = 3 - tap
                moved = pltpu.roll(window, back, 0) if back else window
                filtered = filtered + moved[16:] * conv[tap : tap + 1, lanes]
            smoothed = filtered.astype(BF16)
            logits = jnp.dot(smoothed, gate_pair[g], preferred_element_type=F32)
            rate = jax.nn.sigmoid(logits[:, :128])
            admit = jax.nn.sigmoid(logits[:, 128:])
            rows = pl.ds(start, SEG)
            log_keep = -8.0 * step[rows, lanes] * rate * decay[0:1, lanes]
            kept = jnp.exp(log_keep)
            lost = -2.0 * log_keep
            gap = jnp.where(lost < 0.5, one_minus_exp(jnp.minimum(lost, 0.5)), 1.0 - kept * kept)
            spread = pl.ds(pl.multiple_of(block * PITCH, 8), SEG)
            keep[g, spread, :] = kept
            drive[g, spread, :] = jnp.sqrt(gap) * admit * smoothed.astype(F32)

    def gates_step(block, carry):
        gates(block)
        return carry

    with scope("gates"):
        lax.fori_loop(1, ROWS // SEG, gates_step, 0)

    with scope("load_wait"):
        loads["up"].wait()
        loads["down"].wait()
    with scope("barrier"):
        pl.semaphore_wait(barrier, len(greeted))

    halo = go(value.at[pl.ds(ROWS, 16)], value.at[pl.ds(0, 16)], next_row)

    swaps = []

    def swap(ref):
        swaps.append(go(ref, ref, partner))

    def zz(distance):
        return (z + NZ + distance) % NZ

    def xx(distance):
        return (x + NX + distance) % NX

    own_up = up_w.at[z, x, c]
    own_down = down_w.at[z, x, c]
    up_x = [go(own_up, own_up, x_up), go(own_up, own_up, x_dn)]
    down_z = {(1, 0): go(own_down, own_down, z_up), (1, 1): go(own_down, own_down, z_dn)}
    up_z = {}
    down_x = {}

    def event_up_x1():
        up_x[0].wait_recv()
        ref = up_w.at[z, xx(-1), c, pl.ds(0, 16)]
        up_x.append(go(ref, ref, x_up))
        up_x[1].wait_recv()
        ref = up_w.at[z, xx(1), c, pl.ds(16, 16)]
        up_x.append(go(ref, ref, x_dn))

    def event_up_x2():
        up_x[2].wait_recv()
        up_x[3].wait_recv()
        for h in range(2):
            ref = up_w.at[z, pl.ds(2 * h, 2), c]
            up_z[1, h, 0] = go(ref, ref, z_up)
            up_z[1, h, 1] = go(ref, ref, z_dn)
        swap(up_w.at[z, :, c])

    def event_up_z(d, h):
        def run():
            for way, device, sign in ((0, z_up, -1), (1, z_dn, 1)):
                if (d, h, way) not in up_z:
                    continue
                up_z[d, h, way].wait_recv()
                ref = up_w.at[zz(sign * d), pl.ds(2 * h, 2), c]
                if d < 3 or (d == 3 and h == way):
                    up_z[d + 1, h, way] = go(ref, ref, device)
                swap(ref)

        return run

    def start_down_x(k, zk):
        ref = down_w.at[zk, x, c]
        down_x[k] = [go(ref, ref, x_up), go(ref, ref, x_dn), zk]

    def event_down_z(d):
        def run():
            for way, device, sign in ((0, z_up, -1), (1, z_dn, 1)):
                down_z[d, way].wait_recv()
                source = zz(sign * d)
                if d < 3:
                    ref = down_w.at[source, x, c]
                    down_z[d + 1, way] = go(ref, ref, device)
                elif d == 3:
                    ref = down_w.at[source, x, c, pl.ds(16 * way, 16)]
                    down_z[d + 1, way] = go(ref, ref, device)
                if d < 4:
                    start_down_x(2 * d - 1 + way, source)
            if d == 4:
                start_down_x(7, zz(4))

        return run

    def event_down_x(k):
        def run():
            first, second, zk = down_x[k]
            first.wait_recv()
            if k % 2 == 0:
                ref = down_w.at[zk, xx(-1), c]
                last = go(ref, ref, x_up)
            second.wait_recv()
            if k % 2 == 1:
                ref = down_w.at[zk, xx(1), c]
                last = go(ref, ref, x_dn)
            down_x[k].append(last)

        return run

    def event_down_x2(k):
        def run():
            down_x[k][3].wait_recv()
            swap(down_w.at[down_x[k][2], :, c])

        return run

    events = [
        event_up_x1,
        lambda: start_down_x(0, z),
        event_down_z(1),
        event_up_x2,
        event_down_z(2),
        event_down_x(0),
        event_down_x2(0),
        event_down_x(1),
        event_down_z(3),
        event_up_z(1, 0),
        event_down_x2(1),
        event_down_x(2),
        event_down_z(4),
        event_up_z(1, 1),
        event_down_x2(2),
        event_down_x(3),
        event_up_z(2, 0),
        event_down_x2(3),
        event_down_x(4),
        event_up_z(2, 1),
        event_down_x2(4),
        event_down_x(5),
        event_up_z(3, 0),
        event_down_x2(5),
        event_down_x(6),
        event_up_z(3, 1),
        event_down_x2(6),
        event_down_x(7),
        event_down_x2(7),
        event_up_z(4, 0),
        event_up_z(4, 1),
    ]

    total_events = len(events)

    def pump(count):
        for _ in range(count):
            if events:
                with scope(f"event_{total_events - len(events)}"):
                    events.pop(0)()

    with scope("halo"):
        halo.wait_recv()

    @pl.when(line == 0)
    def _():
        value[0:16, :] = jnp.zeros((16, CH), BF16)

    gates(0)

    def scan_step(t, carry):
        rows = pl.ds(t, 8, stride=PITCH)
        after = []
        for g in range(4):
            product, state = carry[g]
            kept = keep[g, rows, :]
            product = product * kept
            state = kept * state + drive[g, rows, :]
            keep[g, rows, :] = product
            drive[g, rows, :] = state
            after.append((product, state))
        return tuple(after)

    fresh_carry = (jnp.ones((8, 128), F32), jnp.zeros((8, 128), F32))
    with scope("scan"):
        ends = lax.fori_loop(0, SEG, scan_step, (fresh_carry,) * 4, unroll=4)
    for g in range(4):
        product, state = ends[g]
        total_p, total_s = jnp.ones((1, 128), F32), jnp.zeros((1, 128), F32)
        for s in range(8):
            entry_p[g, s : s + 1, :] = total_p
            entry_s[g, s : s + 1, :] = total_s
            total_s = product[s : s + 1] * total_s + state[s : s + 1]
            total_p = total_p * product[s : s + 1]
        pay[g : g + 1, :] = total_p
        pay[g + 4 : g + 5, :] = total_s

    own_plane = x * NC + c
    plane[own_plane] = pay[...]
    in_plane = [go(pay, plane.at[own_plane], device) for device in plane_peers]
    pump(3)
    loads["gate"].wait()

    def gelu_step(block, carry):
        rows = pl.ds(pl.multiple_of(block * SEG, SEG), SEG)
        gelu[rows, :] = jax.nn.gelu(gate[rows, :].astype(F32), approximate=True)
        return carry

    with scope("gelu"):
        lax.fori_loop(0, ROWS // SEG, gelu_step, 0)
    with scope("plane"):
        for copy in in_plane:
            copy.wait_recv()

    def prefix(pieces, size, index):
        run_p, run_s = jnp.ones((4, 128), F32), jnp.zeros((4, 128), F32)
        before_p, before_s = run_p, run_s
        for k in range(size):
            before_p = jnp.where(k == index, run_p, before_p)
            before_s = jnp.where(k == index, run_s, before_s)
            piece = pieces[k]
            run_s = piece[0:4] * run_s + piece[4:8]
            run_p = run_p * piece[0:4]
        return before_p, before_s, run_p, run_s

    inside_p, inside_s, run_p, run_s = prefix(plane, NX * NC, own_plane)
    pay_z[0:4, :] = run_p
    pay_z[4:8, :] = run_s
    column[z] = pay_z[...]
    in_column = [go(pay_z, column.at[z], device) for device in column_peers]
    pump(3)
    with scope("column"):
        for copy in in_column:
            copy.wait_recv()
    _, outer_s, _, _ = prefix(column, NZ, z)
    carried = inside_p * outer_s + inside_s
    for g in range(4):
        entry_s[g] = entry_s[g] + entry_p[g] * carried[g : g + 1]

    for s in range(8):
        rows = pl.ds(s * SEG, SEG)
        for g in range(4):
            lanes = pl.ds(g * 128, 128)
            spread = pl.ds(s * PITCH, SEG)
            hidden = drive[g, spread, :] + keep[g, spread, :] * entry_s[g, s : s + 1, :]
            gated[s % 2, s // 2, :, lanes] = (gelu[rows, lanes] * hidden).astype(BF16)

    left, right = pl.ds(0, HALF), pl.ds(HALF, HALF)

    def scatter_start(pieces, slot):
        return {
            "l1": go(pieces.at[y_op_k, :, left], first_l.at[slot], y_dn),
            "r1": go(pieces.at[y_op_k, :, right], first_r.at[slot], y_up),
            "l0": go(pieces.at[y_up_k, :, left], from_dn.at[slot, :, left], y_up),
            "r0": go(pieces.at[y_dn_k, :, right], from_up.at[slot, :, right], y_dn),
        }

    def scatter_pass(pieces, slot, ring):
        ring["l1"].wait_recv()
        comb_l[slot] = (
            pieces[y_dn_k, :, left].astype(F32) + first_l[slot].astype(F32)
        ).astype(BF16)
        ring["l2"] = go(comb_l.at[slot], from_up.at[slot, :, left], y_dn)
        ring["r1"].wait_recv()
        comb_r[slot] = (
            pieces[y_up_k, :, right].astype(F32) + first_r[slot].astype(F32)
        ).astype(BF16)
        ring["r2"] = go(comb_r.at[slot], from_dn.at[slot, :, right], y_up)

    def scatter_end(pieces, slot, ring):
        for name in ("l0", "r0", "l2", "r2"):
            ring[name].wait_recv()
        return (
            pieces[y].astype(F32) + from_dn[slot].astype(F32) + from_up[slot].astype(F32)
        )

    def gather_start(rows):
        l, r = rows.at[y, :, left], rows.at[y, :, right]
        return [go(l, l, y_up), go(r, r, y_dn), go(r, r, y_up), go(l, l, y_dn)]

    def gather_pass(rows, ring):
        ring[0].wait_recv()
        ref = rows.at[y_dn_k, :, left]
        ring.append(go(ref, ref, y_up))
        ring[1].wait_recv()
        ref = rows.at[y_up_k, :, right]
        ring.append(go(ref, ref, y_dn))

    def gather_end(ring):
        for copy in ring[2:]:
            copy.wait_recv()

    loads["out_w"].wait()

    def project(q):
        rows = gated[q].reshape(4 * SEG, CH)

        def tile_step(n, carry):
            cols = pl.ds(pl.multiple_of(n * TILE, TILE), TILE)
            tile = jnp.dot(rows, out_w[:, cols], preferred_element_type=F32).astype(BF16)
            mixed[q, :, :, cols] = tile.reshape(4, SEG, TILE)
            return carry

        lax.fori_loop(0, D // TILE, tile_step, 0)

    def settle(q, ring):
        total = scatter_end(mixed.at[q], q, ring)
        fresh = (residual[pl.ds(q * SEG, SEG), :].astype(F32) + total).astype(BF16)
        updated[pl.ds(q * SEG, SEG), :] = fresh
        wide = fresh.astype(F32)
        factor = lax.rsqrt(jnp.mean(wide * wide, axis=-1, keepdims=True) + 1e-06)
        normed[q, y] = (wide * factor * gain[...]).astype(BF16)

    loads["residual"].wait()
    loads["gain"].wait()
    def phase(name, call, *args):
        with scope(name):
            return call(*args)

    phase("project0", project, 0)
    ring0 = scatter_start(mixed.at[0], 0)
    phase("project1", project, 1)
    pump(2)
    phase("pass0", scatter_pass, mixed.at[0], 0, ring0)
    ring1 = scatter_start(mixed.at[1], 1)
    pump(6)
    phase("settle0", settle, 0, ring0)
    gather0 = gather_start(normed.at[0])
    phase("pass1", scatter_pass, mixed.at[1], 1, ring1)
    pump(6)
    phase("gpass0", gather_pass, normed.at[0], gather0)
    phase("settle1", settle, 1, ring1)
    gather1 = gather_start(normed.at[1])
    pump(6)
    phase("gend0", gather_end, gather0)
    phase("gpass1", gather_pass, normed.at[1], gather1)
    pump(100)
    with scope("swaps"):
        for copy in swaps:
            copy.wait_recv()

    def feed(q):
        rows = normed[q].reshape(4 * SEG, D)

        def up_step(n, carry):
            cols = pl.ds(pl.multiple_of(n * TILE, TILE), TILE)
            weight = up_w[:, :, :, :, cols].reshape(D, TILE)
            lifted = jnp.maximum(jnp.dot(rows, weight, preferred_element_type=F32), 0.0)
            act[:, cols] = (lifted * lifted).astype(BF16)
            return carry

        lax.fori_loop(0, F // TILE, up_step, 0)
        lhs = act[...]

        def down_step(n, carry):
            cols = pl.ds(pl.multiple_of(n * TILE, TILE), TILE)
            weight = down_w[pl.ds(2 * n, 2)].reshape(TILE, F)
            tile = lax.dot_general(
                lhs, weight, (((1,), (1,)), ((), ())), preferred_element_type=F32
            )
            part[q, :, :, cols] = tile.astype(BF16).reshape(4, SEG, TILE)
            return carry

        lax.fori_loop(0, D // TILE, down_step, 0)

    def close(q, ring):
        total = scatter_end(part.at[q], 2 + q, ring)
        rows = pl.ds(q * SEG, SEG)
        result[rows, :] = (updated[rows, :].astype(F32) + total).astype(BF16)

    phase("feed0", feed, 0)
    ring2 = scatter_start(part.at[0], 2)
    phase("gend1", gather_end, gather1)
    phase("feed1", feed, 1)
    phase("pass2", scatter_pass, part.at[0], 2, ring2)
    ring3 = scatter_start(part.at[1], 3)
    phase("close0", close, 0, ring2)
    phase("pass3", scatter_pass, part.at[1], 3, ring3)
    phase("close1", close, 1, ring3)
    store = pltpu.make_async_copy(result, result_hbm, local_sem.at[len(loads)])
    store.start()
    with scope("finish"):
        copies.finish()
        store.wait()


def local(
    residual_in,
    gate_in,
    value_in,
    conv_weight,
    rate_weight,
    input_weight,
    decay_base,
    step_scale,
    out_weight,
    norm_gain,
    up_weight,
    down_weight,
):
    vmem = pltpu.VMEM
    scratch = [
        vmem((ROWS + 16, CH), BF16),
        vmem((ROWS, CH), BF16),
        vmem((ROWS, CH), F32),
        vmem((4, CH), F32),
        vmem((8, 64, 64), BF16),
        vmem((8, 64, 64), BF16),
        vmem((1, CH), F32),
        vmem((CH, D), BF16),
        vmem((1, D), F32),
        vmem((128, D), BF16),
        vmem((NZ, NX, NC, 32, F), BF16),
        vmem((NZ, NX, NC, 32, F), BF16),
        vmem((4, 128, 256), BF16),
        vmem((4, 8 * PITCH, 128), F32),
        vmem((4, 8 * PITCH, 128), F32),
        vmem((ROWS, CH), F32),
        vmem((4, 8, 128), F32),
        vmem((4, 8, 128), F32),
        vmem((8, 128), F32),
        vmem((NX * NC, 8, 128), F32),
        vmem((8, 128), F32),
        vmem((NZ, 8, 128), F32),
        vmem((2, 4, SEG, CH), BF16),
        vmem((2, 4, SEG, D), BF16),
        vmem((2, 4, SEG, D), BF16),
        vmem((4 * SEG, F), BF16),
        vmem((2, 4, SEG, D), BF16),
        vmem((4, SEG, HALF), BF16),
        vmem((4, SEG, HALF), BF16),
        vmem((4, SEG, HALF), BF16),
        vmem((4, SEG, HALF), BF16),
        vmem((4, SEG, D), BF16),
        vmem((4, SEG, D), BF16),
        vmem((128, D), BF16),
        vmem((128, D), BF16),
        pltpu.SemaphoreType.DMA((16,)),
        pltpu.SemaphoreType.DMA((N_COPIES,)),
        pltpu.SemaphoreType.DMA((N_COPIES,)),
    ]
    return pl.pallas_call(
        kernel,
        out_shape=jax.ShapeDtypeStruct((128, D), BF16),
        in_specs=[pl.BlockSpec(memory_space=pl.ANY)] * 12,
        out_specs=pl.BlockSpec(memory_space=pl.ANY),
        scratch_shapes=scratch,
        compiler_params=pltpu.CompilerParams(
            collective_id=0, has_side_effects=True, vmem_limit_bytes=62 * 1024 * 1024
        ),
    )(
        residual_in,
        gate_in,
        value_in,
        conv_weight,
        rate_weight,
        input_weight,
        decay_base.reshape(1, -1),
        step_scale,
        out_weight,
        norm_gain.reshape(1, -1),
        up_weight,
        down_weight,
    )


def solution(mesh):
    split = Mesh(mesh.devices.reshape(NZ, NX, NC, NY), ("z", "x", "c", "y"))
    return jax.shard_map(
        local,
        mesh=split,
        in_specs=(
            P(SP, None),
            P(SP, "y"),
            P(SP, "y"),
            P(None, "y"),
            P("y", None, None),
            P("y", None, None),
            P("y"),
            P(SP, "y"),
            P("y", None),
            P(),
            P(SP, "y"),
            P(SP, "y"),
        ),
        out_specs=P(SP_TP, None),
        check_vma=False,
    )
```
